512 devices in a mesh: sp: 64 (over z, y), tp: 8 (over x, core).
Axes of the slice: x: 4, y: 4, z: 16, core: 2. Of those that a mesh axis runs over, the one named last changes fastest.
Arguments:
- queries: bfloat16 [12288, 1024], P('sp', 'tp'), may hold values from -6 to 6
- keys: bfloat16 [12288, 512], P('sp', 'tp'), may hold values from -6 to 6
- values: bfloat16 [12288, 512], P('sp', 'tp'), may hold values from -6 to 6
- q_gain: float32 [64], replicated, may hold values from 0.1 to 6.5
- k_gain: float32 [64], replicated, may hold values from 0.1 to 6.5
- w_out: bfloat16 [1024, 2048], P('tp'), may hold values from -12 to 12
- residual: bfloat16 [12288, 2048], P(('sp', 'tp')), may hold values from -6 to 6
- norm_gain: float32 [2048], replicated, may hold values from 0.1 to 1.9
- w_gate: bfloat16 [2048, 5632], P('sp', 'tp'), may hold values from -0.125 to 0.125
- w_up: bfloat16 [2048, 5632], P('sp', 'tp'), may hold values from -0.125 to 0.125
- w_down: bfloat16 [5632, 2048], P('tp', 'sp'), may hold values from -0.25 to 0.25
Outputs:
- layer_out: bfloat16 [12288, 2048], P(('sp', 'tp'))
The draws below stay inside these ranges and needn't reach their ends.
All inputs are finite; a program needn't handle non-finite values.
Results may differ from the reference program's by a relative error of at most 0.018.
The reference program's roundings to bfloat16 on the way count: a program that leaves them out, or rounds other values in their place, can miss the bound.
Values may be sent and summed in bfloat16 or wider, within the bound.
A program may use at most 64 MiB of HBM per device.

```python
import math
import jax
import jax.numpy as jnp
from jax import lax

D = 2048
FF = 5632
HEADS = 16
KV_HEADS = 8
HEAD = 64
GRID_W = 128
TOKENS = 12288
ATTN = 1024
KV_WIDTH = 512


def draw_queries(key, part):
    base = jnp.clip(jax.random.normal(jax.random.fold_in(key, 11), (TOKENS, HEADS * HEAD), jnp.float32), -6.0, 6.0)
    return base.astype(jnp.bfloat16)


def draw_keys(key, part):
    base = jnp.clip(jax.random.normal(jax.random.fold_in(key, 23), (TOKENS, KV_HEADS * HEAD), jnp.float32), -6.0, 6.0)
    return base.astype(jnp.bfloat16)


def draw_q_gain(key, part):
    return jax.random.uniform(jax.random.fold_in(key, 53), (HEAD,), jnp.float32, 0.1, 1.9)


def draw_k_gain(key, part):
    return jax.random.uniform(jax.random.fold_in(key, 63), (HEAD,), jnp.float32, 0.1, 1.9)


def draw_w_out(key, part):
    base = jax.random.normal(jax.random.fold_in(key, 71), (HEADS * HEAD, D), jnp.float32)
    return jnp.clip(base * 2.0, -12.0, 12.0).astype(jnp.bfloat16)


def steps_of(stream_key, shape, cuts, least, largest):
    def one(axis_at, blocks):
        steps = jax.random.uniform(jax.random.fold_in(jax.random.fold_in(stream_key, 6), axis_at), (blocks,), jnp.float32, least / len(cuts), largest / len(cuts))
        return jnp.repeat(jnp.exp(steps), shape[axis_at] // blocks).reshape((-1,) + (1,) * (len(shape) - axis_at - 1))

    factor_of = one(*cuts[0])
    for cut in cuts[1:]:
        factor_of = factor_of * one(*cut)
    return factor_of


def centred(rng, shape, spread, limit, shards=(), held_as=jnp.bfloat16):
    factor_of = steps_of(rng, shape, shards, -0.22, 0.18) if shards else 1.0
    array = jax.random.normal(rng, shape, jnp.float32) * spread * factor_of
    return jnp.minimum(jnp.maximum(array, -limit), limit).astype(held_as)


def setup_inputs(seed: int = 0) -> dict:
    splits = jax.random.split(jax.random.key(seed), 12)
    return {
        "queries": draw_queries(jax.random.fold_in(splits[11], 71), 0),
        "keys": draw_keys(jax.random.fold_in(splits[11], 71), 0),
        "values": centred(splits[2], (TOKENS, KV_WIDTH), 1.0, 6.0, ((0, 64), (1, 8))),
        "q_gain": draw_q_gain(jax.random.fold_in(splits[11], 71), 0),
        "k_gain": draw_k_gain(jax.random.fold_in(splits[11], 71), 0),
        "w_out": draw_w_out(jax.random.fold_in(splits[11], 71), 0),
        "residual": centred(splits[6], (TOKENS, D), 1.0, 6.0, ((0, 512),)),
        "norm_gain": jnp.clip(1.0 + 0.18 * jax.random.normal(splits[7], (D,), jnp.float32), 0.1, 1.9),
        "w_gate": centred(splits[8], (D, FF), D ** -0.5, 0.125, ((0, 64), (1, 8))),
        "w_up": centred(splits[9], (D, FF), D ** -0.5, 0.125, ((0, 64), (1, 8))),
        "w_down": centred(splits[10], (FF, D), (FF // 9) ** -0.5, 0.25, ((0, 8), (1, 64))),
    }


EPS = 1e-06
THETA = 10000.0

def turn_half(part, angle):
    quarter = part.shape[-1] // 2
    cos_table = jnp.cos(angle)[:, None, :]
    sin_table = jnp.sin(angle)[:, None, :]
    first_part = part[..., :quarter]
    second_part = part[..., quarter:]
    return jnp.concatenate([first_part * cos_table - second_part * sin_table, first_part * sin_table + second_part * cos_table], axis=-1)

def head_norm_rope(flat, gain, offset, head_count):
    tok_rows = flat.shape[0]
    head_size = flat.shape[1] // head_count
    heads = flat.astype(jnp.float32).reshape(tok_rows, head_count, head_size)
    heads = heads * lax.rsqrt(lax.optimization_barrier(jnp.mean(heads * heads, axis=-1, keepdims=True)) + EPS) * gain.astype(jnp.float32)
    positions = offset + jnp.arange(tok_rows, dtype=jnp.int32)
    row_pos = (positions // GRID_W).astype(jnp.float32)
    col_pos = (positions % GRID_W).astype(jnp.float32)
    half_size = head_size // 2
    inv_freq = THETA ** (-jnp.arange(0, half_size, 2, dtype=jnp.float32) / half_size)
    turned = jnp.concatenate([turn_half(heads[..., :half_size], row_pos[:, None] * inv_freq[None, :]), turn_half(heads[..., half_size:], col_pos[:, None] * inv_freq[None, :])], axis=-1)
    return turned.reshape(tok_rows, head_count * head_size).astype(jnp.bfloat16)

def reference(queries, keys, values, q_gain, k_gain, w_out, residual, norm_gain, w_gate, w_up, w_down):
    q_group = HEADS // KV_HEADS
    q_rot = head_norm_rope(queries, q_gain, 0, HEADS)
    k_rot = head_norm_rope(keys, k_gain, 0, KV_HEADS)
    key_heads = k_rot.reshape(TOKENS, KV_HEADS, HEAD).astype(jnp.float32)
    value_heads = values.reshape(TOKENS, KV_HEADS, HEAD).astype(jnp.float32)
    block_len = math.gcd(TOKENS, 256)
    query_blocks = q_rot.reshape(TOKENS // block_len, block_len, KV_HEADS, q_group, HEAD)
    score_scale = HEAD ** (-0.5)

    def attend_block(query_block):
        scores = jnp.einsum('qhgd,khd->hgqk', query_block.astype(jnp.float32), key_heads) * score_scale
        top = lax.optimization_barrier(jnp.max(scores, axis=-1, keepdims=True))
        weights = jnp.exp(scores - top)
        totals = lax.optimization_barrier(jnp.sum(weights, axis=-1))
        rounded = weights.astype(jnp.bfloat16).astype(jnp.float32)
        mixed = jnp.einsum('hgqk,khd->qhgd', rounded, value_heads)
        mixed = mixed / jnp.transpose(totals, (2, 0, 1))[..., None]
        return mixed.astype(jnp.bfloat16).reshape(block_len, ATTN)
    attn = lax.map(attend_block, query_blocks).reshape(TOKENS, ATTN)
    proj = jnp.dot(attn, w_out, preferred_element_type=jnp.float32)
    mid = residual.astype(jnp.float32) + proj
    normed = (mid * lax.rsqrt(lax.optimization_barrier(jnp.mean(mid * mid, axis=-1, keepdims=True)) + EPS) * norm_gain.astype(jnp.float32)).astype(jnp.bfloat16)
    gate = jnp.dot(normed, w_gate, preferred_element_type=jnp.float32)
    up_part = jnp.dot(normed, w_up, preferred_element_type=jnp.float32)
    hidden = (jax.nn.silu(gate) * up_part).astype(jnp.bfloat16)
    down = jnp.dot(hidden, w_down, preferred_element_type=jnp.float32)
    return (mid + 0.5 * down).astype(jnp.bfloat16)
```

```python
import jax
import jax.numpy as jnp
from jax import lax
from jax.experimental import pallas as pl
from jax.experimental.pallas import tpu as pltpu
from jax.sharding import Mesh
from jax.sharding import PartitionSpec as P

GRID_W = 128
EPS = 1e-06
THETA = 10000.0
NZ, NY, NX, NC = 16, 4, 4, 2
TOK = 192
ROWS = 24
DM = 2048
HID = 704
UNITS = HID // NY
F32 = jnp.float32
BF16 = jnp.bfloat16
PARTS = ((0, 272), (272, 256))


def nt(a, b):
    return lax.dot_general(a, b, (((1,), (1,)), ((), ())), preferred_element_type=F32)


def norm_rope(h, gain, tab):
    n = h * lax.rsqrt(jnp.mean(h * h, axis=0, keepdims=True) + EPS) * gain
    cr, sr, cc, sc = tab[0:16], tab[16:32], tab[32:48], tab[48:64]
    a, b, c, d = n[0:16], n[16:32], n[32:48], n[48:64]
    return jnp.concatenate([a * cr - b * sr, a * sr + b * cr, c * cc - d * sc, c * sc + d * cc], axis=0)


def kernel(
    q_ref, kt_ref, vt_ref, tab_ref, wg_ref, wu_ref, wdt_ref, wout_ref, res_ref, ng_ref, out_ref,
    kv, qa, kk, vv, mx0, mx1, ls0, ls1, acc, wt, wp, ws, wm, wo, rs_, aa, osend, orecv, ssend, srecv,
    mid, nb, dn, pown, dsend, drecv, rsend, rrecv, mown, osum,
    kvs, kvr, qs, qr, wps, wpr, wrs, wrr, r1s, r1r, r2s, r2r, rds, rdr, wos, wor, wds, wdr,
    os_, or_, ss_, sr_, as_, ar_, ads, adr, dds, ddr, fs, fr,
):
    z, y, x, c = (lax.axis_index(n) for n in ("z", "y", "x", "c"))
    tp = x * 2 + c
    pending = []

    def go(src, dst, ssem, rsem, dev):
        cp = pltpu.make_async_remote_copy(
            src_ref=src, dst_ref=dst, send_sem=ssem, recv_sem=rsem, device_id=dev, device_id_type=pl.DeviceIdType.MESH
        )
        cp.start()
        pending.append(cp)

    def got(dst, ssem, rsem):
        pltpu.make_async_remote_copy(
            src_ref=dst, dst_ref=dst, send_sem=ssem, recv_sem=rsem, device_id=(z, y, x, c), device_id_type=pl.DeviceIdType.MESH
        ).wait_recv()

    def up(v, d, n):
        return lax.rem(v + d + n, n)

    def lanes(i):
        return pl.ds(pl.multiple_of(i * 128, 128), 128)

    partner = (z, y, x, 1 - c)
    znext, zprev = (up(z, 1, NZ), y, x, c), (up(z, -1, NZ), y, x, c)

    bar = pltpu.get_barrier_semaphore()
    peers = [partner, znext, zprev]
    for d in range(NY):
        for e in range(NX):
            if d or e:
                peers.append((z, up(y, d, NY), up(x, e, NX), c))
    for p in peers:
        pl.semaphore_signal(bar, inc=1, device_id=p, device_id_type=pl.DeviceIdType.MESH)

    tab = tab_ref[...]
    kr = norm_rope(kt_ref[...].astype(F32), tab[128:192], tab)
    kv[0] = jnp.concatenate([kr, vt_ref[...].astype(F32)], axis=0).T.astype(BF16)
    qt = q_ref[...].astype(F32).T
    qr2 = jnp.concatenate([norm_rope(qt[0:64], tab[64:128], tab), norm_rope(qt[64:128], tab[64:128], tab)], axis=0)
    qa[y] = (qr2.T * 0.125).astype(BF16)
    w4 = jnp.concatenate(
        [wg_ref[...].astype(F32), wu_ref[...].astype(F32), wdt_ref[...].astype(F32), jnp.zeros((32, HID), F32)], axis=0
    )
    wt[...] = w4.T
    for d in range(NY):
        yb = up(y, d, NY)
        piece = wt[pl.ds(pl.multiple_of(yb * UNITS, 8), UNITS), :].astype(BF16)
        if d == 0:
            wp[y] = piece
        else:
            ws[d - 1] = piece
    pl.semaphore_wait(bar, len(peers))

    def kv_cw(s):
        go(kv.at[0 if s == 0 else 2 * s - 1], kv.at[2 * s + 1], kvs.at[0, s], kvr.at[0, s], znext)

    def kv_ccw(s):
        go(kv.at[2 * s], kv.at[2 * s + 2], kvs.at[1, s], kvr.at[1, s], zprev)

    kv_cw(0)
    kv_ccw(0)
    for d in range(1, NY):
        dev = (z, up(y, d, NY), x, c)
        go(qa.at[y], qa.at[y], qs.at[d - 1], qr.at[d - 1], dev)
    for d in range(1, NY):
        dev = (z, up(y, d, NY), x, c)
        go(ws.at[d - 1], wp.at[y], wps.at[d - 1], wpr.at[d - 1], dev)
    for e in range(1, NX):
        dev = (z, y, up(x, e, NX), c)
        go(res_ref, rs_.at[c, y, x], r1s.at[e - 1], r1r.at[e - 1], dev)
    wrow = pl.ds(pl.multiple_of(tp * 128, 128), 128)
    for e in range(1, NX):
        dev = (z, y, up(x, e, NX), c)
        go(wout_ref, wo.at[wrow], wos.at[e - 1], wor.at[e - 1], dev)
    go(wout_ref, wo.at[wrow], wds.at[0], wdr.at[0], partner)
    wo[wrow] = wout_ref[...]
    rs_[c, y, x] = res_ref[...]

    def w_slice(part, blk):
        r0, nr = PARTS[part]
        return wm.at[pl.ds(r0, nr), lanes(blk)]

    def w_send(part, j, way):
        sl = w_slice(part, up(z, -j if way == 0 else j, NZ))
        go(sl, sl, wrs.at[way, part, j], wrr.at[way, part, j], znext if way == 0 else zprev)

    def pump(t):
        part, j = t % 2, t // 2
        for way, last in ((0, 8), (1, 7)):
            if j < last:
                sl = w_slice(part, up(z, -1 - j if way == 0 else 1 + j, NZ))
                got(sl, wrs.at[way, part, j], wrr.at[way, part, j])
                if j + 1 < last:
                    w_send(part, j + 1, way)

    lane = lax.broadcasted_iota(jnp.int32, (UNITS, 128), 1)

    def w_start():
        for d in range(1, NY):
            got(wp.at[up(y, -d, NY)], wps.at[d - 1], wpr.at[d - 1])
        pieces = [wp[i].astype(F32) for i in range(NY)]
        for m in range(3):
            blk = None
            for i in range(NY):
                sh = (32 * (i - m)) % 128
                r = pltpu.roll(pieces[i], sh, 1) if sh else pieces[i]
                blk = r if blk is None else jnp.where(lane >= 32 * i, r, blk)
            wm[pl.ds(m * UNITS, UNITS), lanes(z)] = blk.astype(BF16)
        for part in range(2):
            w_send(part, 0, 0)
            w_send(part, 0, 1)

    for d in range(1, NY):
        got(qa.at[up(y, -d, NY)], qs.at[d - 1], qr.at[d - 1])
    mx0[...] = jnp.full(mx0.shape, -1e30, F32)
    mx1[...] = jnp.full(mx1.shape, -1e30, F32)
    ls0[...] = jnp.zeros(ls0.shape, F32)
    ls1[...] = jnp.zeros(ls1.shape, F32)
    acc[...] = jnp.zeros(acc.shape, F32)

    low = lax.broadcasted_iota(jnp.int32, (2 * TOK, 128), 1) < 64
    clow = lax.broadcasted_iota(jnp.int32, (128, 128), 1) < 64

    def attend(s):
        both = jnp.concatenate([kv[2 * s], kv[2 * s + 1]], axis=0).astype(F32)
        turned = pltpu.roll(both, 64, 1)
        none = jnp.zeros_like(both)
        kk[0 : 2 * TOK] = jnp.where(low, both, none).astype(BF16)
        kk[2 * TOK : 4 * TOK] = jnp.where(low, none, turned).astype(BF16)
        vv[0 : 2 * TOK] = jnp.where(low, turned, none).astype(BF16)
        vv[2 * TOK : 4 * TOK] = jnp.where(low, none, both).astype(BF16)

        def chunk(i, carry):
            yb = i // 3
            rows = pl.ds(pl.multiple_of(i * 64, 64), 64)
            sub = pl.ds(pl.multiple_of((i - 3 * yb) * 64, 64), 64)
            sc = nt(qa[yb, sub], kk[...])
            probs, facs = [], []
            for h, (mx, ls) in enumerate(((mx0, ls0), (mx1, ls1))):
                cols = [sc[:, 128 * (3 * h + j) : 128 * (3 * h + j + 1)] for j in range(3)]
                old = mx[rows]
                top = jnp.max(jnp.maximum(jnp.maximum(cols[0], cols[1]), cols[2]), axis=1, keepdims=True)
                new = jnp.maximum(old, top)
                fac = jnp.exp(old - new)
                ps = [jnp.exp(v - new) for v in cols]
                ls[rows] = ls[rows] * fac + (ps[0] + ps[1] + ps[2])
                mx[rows] = new
                probs += ps
                facs.append(fac)
            pb = jnp.concatenate([p.astype(BF16) for p in probs], axis=1)
            o = jnp.dot(pb, vv[...], preferred_element_type=F32)
            acc[rows] = acc[rows] * jnp.where(clow[0:64], facs[0], facs[1]) + o
            return carry

        lax.fori_loop(0, 12, chunk, 0)

    for s in range(8):
        got(kv.at[2 * s + 1], kvs.at[0, s], kvr.at[0, s])
        if s < 7:
            kv_cw(s + 1)
            got(kv.at[2 * s + 2], kvs.at[1, s], kvr.at[1, s])
            if s < 6:
                kv_ccw(s + 1)
        if s == 1:
            w_start()
        if s >= 3:
            pump(s - 3)
        if s == 3:
            for e in range(1, NX):
                got(rs_.at[c, y, up(x, -e, NX)], r1s.at[e - 1], r1r.at[e - 1])
            for d in range(1, NY):
                go(rs_.at[c, y], rs_.at[c, y], r2s.at[d - 1], r2r.at[d - 1], (z, up(y, d, NY), x, c))
            go(rs_.at[c, y], rs_.at[c, y], rds.at[0], rdr.at[0], partner)
        attend(s)

    lane_t = lax.broadcasted_iota(jnp.int32, (TOK, 128), 1)
    tlow = lane_t < 64
    thalf = lax.rem(lane_t, 64) < 32

    def part_of(yb):
        rows = pl.ds(pl.multiple_of(yb * TOK, 64), TOK)
        l0 = jnp.sum(ls0[rows], axis=1, keepdims=True)
        l1 = jnp.sum(ls1[rows], axis=1, keepdims=True)
        lb = jnp.where(tlow, l0, l1)
        mb = jnp.where(tlow, mx0[rows], mx1[rows])
        st = jnp.where(thalf, mb, lb).T
        packed = jnp.concatenate([st[0:8], st[32:40], st[64:72], st[96:104]], axis=0)
        return acc[rows] / lb, packed

    for d in range(1, NY):
        yb = up(y, d, NY)
        o, st = part_of(yb)
        osend[d - 1] = o.astype(BF16)
        ssend[d - 1] = st
        dev = (z, yb, x, c)
        go(ssend.at[d - 1], srecv.at[d - 1], ss_.at[d - 1], sr_.at[d - 1], dev)
        go(osend.at[d - 1], orecv.at[d - 1], os_.at[d - 1], or_.at[d - 1], dev)
    pump(5)
    mine, st = part_of(y)
    outs, stats = [mine], [st]
    for d in range(1, NY):
        got(srecv.at[d - 1], ss_.at[d - 1], sr_.at[d - 1])
        got(orecv.at[d - 1], os_.at[d - 1], or_.at[d - 1])
        outs.append(orecv[d - 1].astype(F32))
        stats.append(srecv[d - 1])
    coef = []
    for h in range(2):
        ms = [s_[16 * h : 16 * h + 8] for s_ in stats]
        top = jnp.maximum(jnp.maximum(ms[0], ms[1]), jnp.maximum(ms[2], ms[3]))
        wts = [s_[16 * h + 8 : 16 * h + 16] * jnp.exp(m - top) for s_, m in zip(stats, ms)]
        tot = (wts[0] + wts[1]) + (wts[2] + wts[3])
        coef.append([w / tot for w in wts])
    attn = None
    for p in range(NY):
        cf = jnp.concatenate([coef[0][p]] * 8 + [coef[1][p]] * 8, axis=0).T
        attn = cf * outs[p] if attn is None else attn + cf * outs[p]

    own = aa.at[y, :, lanes(tp)]
    aa[y, :, lanes(tp)] = attn.astype(BF16)
    for d in range(NY):
        for e in range(NX):
            o = d * NX + e
            if o:
                go(own, own, as_.at[o], ar_.at[o], (z, up(y, d, NY), up(x, e, NX), c))
    go(own, own, ads.at[0], adr.at[0], partner)

    for e in range(1, NX):
        wr = pl.ds(pl.multiple_of((up(x, -e, NX) * 2 + c) * 128, 128), 128)
        got(wo.at[wr], wos.at[e - 1], wor.at[e - 1])
        go(wo.at[wr], wo.at[wr], wds.at[e], wdr.at[e], partner)
    for d in range(1, NY):
        yb = up(y, -d, NY)
        got(rs_.at[c, yb], r2s.at[d - 1], r2r.at[d - 1])
        go(rs_.at[c, yb], rs_.at[c, yb], rds.at[d], rdr.at[d], partner)
    for t in range(6, 10):
        pump(t)
    for d in range(NY):
        for e in range(NX):
            o = d * NX + e
            if o:
                sl = aa.at[up(y, -d, NY), :, lanes(up(x, -e, NX) * 2 + c)]
                got(sl, as_.at[o], ar_.at[o])
                go(sl, sl, ads.at[o], adr.at[o], partner)
    for t in range(10, 16):
        pump(t)
    for e in range(NX):
        wr = pl.ds(pl.multiple_of((up(x, -e, NX) * 2 + 1 - c) * 128, 128), 128)
        got(wo.at[wr], wds.at[e], wdr.at[e])

    gain = ng_ref[...]

    def block(d):
        yb = up(y, -d, NY)
        for e in range(NX):
            sl = aa.at[yb, :, lanes(up(x, -e, NX) * 2 + 1 - c)]
            got(sl, ads.at[d * NX + e], adr.at[d * NX + e])
        got(rs_.at[1 - c, yb], rds.at[d], rdr.at[d])
        for n in range(4):
            cols = slice(512 * n, 512 * n + 512)
            mid[:, cols] = jnp.dot(aa[yb], wo[:, cols], preferred_element_type=F32)
        for t in range(8):
            r = slice(ROWS * t, ROWS * t + ROWS)
            v = mid[r] + rs_[t % 2, yb, t // 2].astype(F32)
            mid[r] = v
            sq = jnp.mean(v * v, axis=1, keepdims=True)
            dn[r] = v * lax.rsqrt(sq + EPS) * gain
        nb[...] = dn[...].astype(BF16)
        if d == 0:
            mown[...] = mid[pl.ds(pl.multiple_of(tp * ROWS, 8), ROWS)]
        g = nt(nb[...], wm[0:UNITS])
        u = nt(nb[...], wm[UNITS : 2 * UNITS])
        hid = (g / (1.0 + jnp.exp(-g)) * u).astype(BF16)
        for n in range(4):
            cols = slice(512 * n, 512 * n + 512)
            dn[:, cols] = jnp.dot(hid, wm[2 * UNITS : 3 * UNITS, cols], preferred_element_type=F32)
        for e in range(NX):
            xb = up(x, -e, NX)
            pown[d * NX + e] = dn[pl.ds(pl.multiple_of((xb * 2 + c) * ROWS, 8), ROWS)]
            dsend[d, e] = dn[pl.ds(pl.multiple_of((xb * 2 + 1 - c) * ROWS, 8), ROWS)].astype(BF16)
        go(dsend.at[d], drecv.at[d], dds.at[d], ddr.at[d], partner)

    def finish(d):
        got(drecv.at[d], dds.at[d], ddr.at[d])
        for e in range(NX):
            o = d * NX + e
            v = pown[o] + drecv[d, e].astype(F32)
            if o == 0:
                osum[...] = v
            else:
                rsend[o] = v.astype(BF16)
                go(rsend.at[o], rrecv.at[o], fs.at[o], fr.at[o], (z, up(y, -d, NY), up(x, -e, NX), c))

    for d in range(NY):
        block(d)
        if d:
            finish(d - 1)
    finish(NY - 1)
    total = osum[...]
    for o in range(1, NX * NY):
        got(rrecv.at[o], fs.at[o], fr.at[o])
        total = total + rrecv[o].astype(F32)
    out_ref[...] = (mown[...] + 0.5 * total).astype(BF16)
    for cp in pending:
        cp.wait_send()


def body(queries, keys, values, q_gain, k_gain, w_out, residual, norm_gain, w_gate, w_up, w_down):
    first = (lax.axis_index("z") * NY + lax.axis_index("y")) * TOK
    positions = first + jnp.arange(TOK, dtype=jnp.int32)
    row_pos = (positions // GRID_W).astype(F32)
    col_pos = (positions % GRID_W).astype(F32)
    inv_freq = THETA ** (-jnp.arange(0, 32, 2, dtype=F32) / 32)
    ar = inv_freq[:, None] * row_pos[None, :]
    ac = inv_freq[:, None] * col_pos[None, :]
    tab = jnp.concatenate(
        [
            jnp.cos(ar), jnp.sin(ar), jnp.cos(ac), jnp.sin(ac),
            jnp.broadcast_to(q_gain[:, None], (64, TOK)),
            jnp.broadcast_to(k_gain[:, None], (64, TOK)),
        ],
        axis=0,
    )
    v = pltpu.VMEM
    dma = pltpu.SemaphoreType.DMA
    scratch = [
        v((NZ, TOK, 128), BF16),
        v((NY, TOK, 128), BF16),
        v((4 * TOK, 128), BF16),
        v((4 * TOK, 128), BF16),
        *[v((NY * TOK, 128), F32)] * 5,
        v((HID, 128), F32),
        v((NY, UNITS, 128), BF16),
        v((NY - 1, UNITS, 128), BF16),
        v((3 * UNITS, DM), BF16),
        v((1024, DM), BF16),
        v((NC, NY, NX, ROWS, DM), BF16),
        v((NY, TOK, 1024), BF16),
        v((3, TOK, 128), BF16), v((3, TOK, 128), BF16),
        v((3, 32, TOK), F32), v((3, 32, TOK), F32),
        v((TOK, DM), F32), v((TOK, DM), BF16), v((TOK, DM), F32),
        v((16, ROWS, DM), F32),
        v((NY, NX, ROWS, DM), BF16), v((NY, NX, ROWS, DM), BF16),
        v((16, ROWS, DM), BF16), v((16, ROWS, DM), BF16),
        v((ROWS, DM), F32), v((ROWS, DM), F32),
        dma((2, 8)), dma((2, 8)), dma((3,)), dma((3,)), dma((3,)), dma((3,)), dma((2, 2, 8)), dma((2, 2, 8)),
        dma((3,)), dma((3,)), dma((3,)), dma((3,)), dma((4,)), dma((4,)), dma((3,)), dma((3,)), dma((4,)), dma((4,)),
        dma((3,)), dma((3,)), dma((3,)), dma((3,)), dma((16,)), dma((16,)), dma((16,)), dma((16,)),
        dma((4,)), dma((4,)), dma((16,)), dma((16,)),
    ]
    return pl.pallas_call(
        kernel,
        out_shape=jax.ShapeDtypeStruct((ROWS, DM), BF16),
        in_specs=[pl.BlockSpec(memory_space=pltpu.VMEM)] * 10,
        out_specs=pl.BlockSpec(memory_space=pltpu.VMEM),
        scratch_shapes=scratch,
        compiler_params=pltpu.CompilerParams(collective_id=0, has_side_effects=True, vmem_limit_bytes=60 * 1024 * 1024),
        name="layer",
    )(queries, keys.T, values.T, tab, w_gate, w_up, w_down.T, w_out, residual, norm_gain[None, :])


def solution(mesh):
    finer = Mesh(mesh.devices.reshape(NZ, NY, NX, NC), ("z", "y", "x", "c"))
    sp, tp, every = ("z", "y"), ("x", "c"), ("z", "y", "x", "c")
    placed = (
        P(sp, tp), P(sp, tp), P(sp, tp), P(), P(), P(tp, None), P(every, None), P(), P(sp, tp), P(sp, tp), P(tp, sp),
    )
    return jax.shard_map(body, mesh=finer, in_specs=placed, out_specs=P(every, None), check_vma=False)
```

```python
import jax
import jax.numpy as jnp
from jax import lax
from jax.experimental import pallas as pl
from jax.experimental.pallas import tpu as pltpu
from jax.sharding import Mesh
from jax.sharding import PartitionSpec as P

GRID_W = 128
EPS = 1e-06
THETA = 10000.0
NZ, NY, NX, NC = 16, 4, 4, 2
TOK = 192
ROWS = 24
DM = 2048
HID = 704
UNITS = HID // NY
F32 = jnp.float32
BF16 = jnp.bfloat16
PARTS = tuple((UNITS * m, UNITS) for m in range(3))


def nt(a, b):
    return lax.dot_general(a, b, (((1,), (1,)), ((), ())), preferred_element_type=F32)


def norm_rope(h, gain, tab):
    n = h * lax.rsqrt(jnp.mean(h * h, axis=0, keepdims=True) + EPS) * gain
    cr, sr, cc, sc = tab[0:16], tab[16:32], tab[32:48], tab[48:64]
    a, b, c, d = n[0:16], n[16:32], n[32:48], n[48:64]
    return jnp.concatenate([a * cr - b * sr, a * sr + b * cr, c * cc - d * sc, c * sc + d * cc], axis=0)


def kernel(
    q_ref, kt_ref, vt_ref, tab_ref, wg_ref, wu_ref, wdt_ref, wout_ref, res_ref, ng_ref, out_ref,
    kv, qa, kk, vv, mx0, mx1, ls0, ls1, acc, wt, wp, ws, wm, wo, rs_, aa, osend, orecv, ssend, srecv,
    mid, nb, dn, pown, dsend, drecv, mown, asend, arecv, aown, bsend, brecv, bown, a2send, a2recv, b2send, b2recv, outa,
    kvs, kvr, qs, qr, wps, wpr, wrs, wrr, r1s, r1r, r2s, r2r, rds, rdr, wos, wor, wds, wdr,
    os_, or_, ss_, sr_, as_, ar_, ads, adr, dds, ddr, f1s, f1r, f2s, f2r, f3s, f3r, f4s, f4r,
):
    z, y, x, c = (lax.axis_index(n) for n in ("z", "y", "x", "c"))
    tp = x * 2 + c
    pending = []

    def go(src, dst, ssem, rsem, dev):
        cp = pltpu.make_async_remote_copy(
            src_ref=src, dst_ref=dst, send_sem=ssem, recv_sem=rsem, device_id=dev, device_id_type=pl.DeviceIdType.MESH
        )
        cp.start()
        pending.append(cp)

    def got(dst, ssem, rsem):
        pltpu.make_async_remote_copy(
            src_ref=dst, dst_ref=dst, send_sem=ssem, recv_sem=rsem, device_id=(z, y, x, c), device_id_type=pl.DeviceIdType.MESH
        ).wait_recv()

    def up(v, d, n):
        return lax.rem(v + d + n, n)

    def lanes(i):
        return pl.ds(pl.multiple_of(i * 128, 128), 128)

    partner = (z, y, x, 1 - c)
    znext, zprev = (up(z, 1, NZ), y, x, c), (up(z, -1, NZ), y, x, c)

    bar = pltpu.get_barrier_semaphore()
    peers = [partner, znext, zprev]
    for d in range(NY):
        for e in range(NX):
            if d or e:
                peers.append((z, up(y, d, NY), up(x, e, NX), c))
    for p in peers:
        pl.semaphore_signal(bar, inc=1, device_id=p, device_id_type=pl.DeviceIdType.MESH)

    tab = tab_ref[...]
    kr = norm_rope(kt_ref[...].astype(F32), tab[128:192], tab)
    kv[0] = jnp.concatenate([kr, vt_ref[...].astype(F32)], axis=0).T.astype(BF16)
    qt = q_ref[...].astype(F32).T
    qr2 = jnp.concatenate([norm_rope(qt[0:64], tab[64:128], tab), norm_rope(qt[64:128], tab[64:128], tab)], axis=0)
    qa[y] = (qr2.T * 0.125).astype(BF16)
    w4 = jnp.concatenate(
        [wg_ref[...].astype(F32), wu_ref[...].astype(F32), wdt_ref[...].astype(F32), jnp.zeros((32, HID), F32)], axis=0
    )
    wt[...] = w4.T
    for d in range(NY):
        yb = up(y, d, NY)
        piece = wt[pl.ds(pl.multiple_of(yb * UNITS, 8), UNITS), :].astype(BF16)
        if d == 0:
            wp[y] = piece
        else:
            ws[d - 1] = piece
    pl.semaphore_wait(bar, len(peers))

    def kv_cw(s):
        go(kv.at[0 if s == 0 else 2 * s - 1], kv.at[2 * s + 1], kvs.at[0, s], kvr.at[0, s], znext)

    def kv_ccw(s):
        go(kv.at[2 * s], kv.at[2 * s + 2], kvs.at[1, s], kvr.at[1, s], zprev)

    kv_cw(0)
    kv_ccw(0)
    for d in range(1, NY):
        dev = (z, up(y, d, NY), x, c)
        go(qa.at[y], qa.at[y], qs.at[d - 1], qr.at[d - 1], dev)
    for d in range(1, NY):
        dev = (z, up(y, d, NY), x, c)
        go(ws.at[d - 1], wp.at[y], wps.at[d - 1], wpr.at[d - 1], dev)
    for e in range(1, NX):
        dev = (z, y, up(x, e, NX), c)
        go(res_ref, rs_.at[c, y, x], r1s.at[e - 1], r1r.at[e - 1], dev)
    wrow = pl.ds(pl.multiple_of(tp * 128, 128), 128)
    for e in range(1, NX):
        dev = (z, y, up(x, e, NX), c)
        go(wout_ref, wo.at[wrow], wos.at[e - 1], wor.at[e - 1], dev)
    go(wout_ref, wo.at[wrow], wds.at[0], wdr.at[0], partner)
    wo[wrow] = wout_ref[...]
    rs_[c, y, x] = res_ref[...]

    def w_slice(part, blk):
        r0, nr = PARTS[part]
        return wm.at[pl.ds(r0, nr), lanes(blk)]

    def w_send(part, j, way):
        sl = w_slice(part, up(z, -j if way == 0 else j, NZ))
        go(sl, sl, wrs.at[way, part, j], wrr.at[way, part, j], znext if way == 0 else zprev)

    def pump(t):
        part, j = t % 3, t // 3
        for way, last in ((0, 8), (1, 7)):
            if j < last:
                sl = w_slice(part, up(z, -1 - j if way == 0 else 1 + j, NZ))
                got(sl, wrs.at[way, part, j], wrr.at[way, part, j])
                if j + 1 < last:
                    w_send(part, j + 1, way)

    lane = lax.broadcasted_iota(jnp.int32, (UNITS, 128), 1)

    def w_start():
        for d in range(1, NY):
            got(wp.at[up(y, -d, NY)], wps.at[d - 1], wpr.at[d - 1])
        pieces = [wp[i].astype(F32) for i in range(NY)]
        for m in range(3):
            blk = None
            for i in range(NY):
                sh = (32 * (i - m)) % 128
                r = pltpu.roll(pieces[i], sh, 1) if sh else pieces[i]
                blk = r if blk is None else jnp.where(lane >= 32 * i, r, blk)
            wm[pl.ds(m * UNITS, UNITS), lanes(z)] = blk.astype(BF16)
        for part in range(3):
            w_send(part, 0, 0)
            w_send(part, 0, 1)

    mx0[...] = jnp.full(mx0.shape, -1e30, F32)
    mx1[...] = jnp.full(mx1.shape, -1e30, F32)
    ls0[...] = jnp.zeros(ls0.shape, F32)
    ls1[...] = jnp.zeros(ls1.shape, F32)
    acc[...] = jnp.zeros(acc.shape, F32)

    low = lax.broadcasted_iota(jnp.int32, (2 * TOK, 128), 1) < 64
    qlow = lax.broadcasted_iota(jnp.int32, (NY * TOK, 128), 1) < 64

    def attend(s):
        both = jnp.concatenate([kv[2 * s], kv[2 * s + 1]], axis=0).astype(F32)
        turned = pltpu.roll(both, 64, 1)
        none = jnp.zeros_like(both)
        kk[0 : 2 * TOK] = jnp.where(low, both, none).astype(BF16)
        kk[2 * TOK : 4 * TOK] = jnp.where(low, none, turned).astype(BF16)
        vv[0 : 2 * TOK] = jnp.where(low, turned, none).astype(BF16)
        vv[2 * TOK : 4 * TOK] = jnp.where(low, none, both).astype(BF16)

        sc = nt(qa[...].reshape(NY * TOK, 128), kk[...])
        probs, facs = [], []
        for h, (mx, ls) in enumerate(((mx0, ls0), (mx1, ls1))):
            cols = [sc[:, 128 * (3 * h + j) : 128 * (3 * h + j + 1)] for j in range(3)]
            old = mx[...]
            top = jnp.max(jnp.maximum(jnp.maximum(cols[0], cols[1]), cols[2]), axis=1, keepdims=True)
            new = jnp.maximum(old, top)
            fac = jnp.exp(old - new)
            ps = [jnp.exp(v - new) for v in cols]
            ls[...] = ls[...] * fac + (ps[0] + ps[1] + ps[2])
            mx[...] = new
            probs += ps
            facs.append(fac)
        pb = jnp.concatenate([p.astype(BF16) for p in probs], axis=1)
        o = jnp.dot(pb, vv[...], preferred_element_type=F32)
        acc[...] = acc[...] * jnp.where(qlow, facs[0], facs[1]) + o

    for s in range(8):
        got(kv.at[2 * s + 1], kvs.at[0, s], kvr.at[0, s])
        if s < 7:
            kv_cw(s + 1)
            got(kv.at[2 * s + 2], kvs.at[1, s], kvr.at[1, s])
            if s < 6:
                kv_ccw(s + 1)
        if s == 0:
            for d in range(1, NY):
                got(qa.at[up(y, -d, NY)], qs.at[d - 1], qr.at[d - 1])
        if s == 1:
            w_start()
        if s >= 2:
            pump(2 * s - 4)
            pump(2 * s - 3)
        if s == 3:
            for e in range(1, NX):
                got(rs_.at[c, y, up(x, -e, NX)], r1s.at[e - 1], r1r.at[e - 1])
            for d in range(1, NY):
                go(rs_.at[c, y], rs_.at[c, y], r2s.at[d - 1], r2r.at[d - 1], (z, up(y, d, NY), x, c))
            go(rs_.at[c, y], rs_.at[c, y], rds.at[0], rdr.at[0], partner)
        attend(s)

    lane_t = lax.broadcasted_iota(jnp.int32, (TOK, 128), 1)
    tlow = lane_t < 64
    thalf = lax.rem(lane_t, 64) < 32

    def part_of(yb):
        rows = pl.ds(pl.multiple_of(yb * TOK, 64), TOK)
        l0 = jnp.sum(ls0[rows], axis=1, keepdims=True)
        l1 = jnp.sum(ls1[rows], axis=1, keepdims=True)
        lb = jnp.where(tlow, l0, l1)
        mb = jnp.where(tlow, mx0[rows], mx1[rows])
        st = jnp.where(thalf, mb, lb).T
        packed = jnp.concatenate([st[0:8], st[32:40], st[64:72], st[96:104]], axis=0)
        return acc[rows] / lb, packed

    for d in range(1, NY):
        yb = up(y, d, NY)
        o, st = part_of(yb)
        osend[d - 1] = o.astype(BF16)
        ssend[d - 1] = st
        dev = (z, yb, x, c)
        go(ssend.at[d - 1], srecv.at[d - 1], ss_.at[d - 1], sr_.at[d - 1], dev)
        go(osend.at[d - 1], orecv.at[d - 1], os_.at[d - 1], or_.at[d - 1], dev)
    pump(12)
    pump(13)
    mine, st = part_of(y)
    outs, stats = [mine], [st]
    for d in range(1, NY):
        got(srecv.at[d - 1], ss_.at[d - 1], sr_.at[d - 1])
        got(orecv.at[d - 1], os_.at[d - 1], or_.at[d - 1])
        outs.append(orecv[d - 1].astype(F32))
        stats.append(srecv[d - 1])
    coef = []
    for h in range(2):
        ms = [s_[16 * h : 16 * h + 8] for s_ in stats]
        top = jnp.maximum(jnp.maximum(ms[0], ms[1]), jnp.maximum(ms[2], ms[3]))
        wts = [s_[16 * h + 8 : 16 * h + 16] * jnp.exp(m - top) for s_, m in zip(stats, ms)]
        tot = (wts[0] + wts[1]) + (wts[2] + wts[3])
        coef.append([w / tot for w in wts])
    attn = None
    for p in range(NY):
        cf = jnp.concatenate([coef[0][p]] * 8 + [coef[1][p]] * 8, axis=0).T
        attn = cf * outs[p] if attn is None else attn + cf * outs[p]

    own = aa.at[y, :, lanes(tp)]
    aa[y, :, lanes(tp)] = attn.astype(BF16)
    for d in range(NY):
        for e in range(NX):
            o = d * NX + e
            if o:
                go(own, own, as_.at[o], ar_.at[o], (z, up(y, d, NY), up(x, e, NX), c))
    go(own, own, ads.at[0], adr.at[0], partner)

    for e in range(1, NX):
        wr = pl.ds(pl.multiple_of((up(x, -e, NX) * 2 + c) * 128, 128), 128)
        got(wo.at[wr], wos.at[e - 1], wor.at[e - 1])
        go(wo.at[wr], wo.at[wr], wds.at[e], wdr.at[e], partner)
    for d in range(1, NY):
        yb = up(y, -d, NY)
        got(rs_.at[c, yb], r2s.at[d - 1], r2r.at[d - 1])
        go(rs_.at[c, yb], rs_.at[c, yb], rds.at[d], rdr.at[d], partner)
    pump(14)
    pump(15)

    def forward(d):
        for e in range(NX):
            o = d * NX + e
            if o:
                sl = aa.at[up(y, -d, NY), :, lanes(up(x, -e, NX) * 2 + c)]
                got(sl, as_.at[o], ar_.at[o])
                go(sl, sl, ads.at[o], adr.at[o], partner)

    gain = ng_ref[...]

    def project(d):
        yb = up(y, -d, NY)
        if d == 0:
            for e in range(NX):
                wr = pl.ds(pl.multiple_of((up(x, -e, NX) * 2 + 1 - c) * 128, 128), 128)
                got(wo.at[wr], wds.at[e], wdr.at[e])
        for e in range(NX):
            sl = aa.at[yb, :, lanes(up(x, -e, NX) * 2 + 1 - c)]
            got(sl, ads.at[d * NX + e], adr.at[d * NX + e])
        got(rs_.at[1 - c, yb], rds.at[d], rdr.at[d])
        for n in range(4):
            cols = slice(512 * n, 512 * n + 512)
            mid[:, cols] = jnp.dot(aa[yb], wo[:, cols], preferred_element_type=F32)
        for t in range(8):
            r = slice(ROWS * t, ROWS * t + ROWS)
            v = mid[r] + rs_[t % 2, yb, t // 2].astype(F32)
            mid[r] = v
            sq = jnp.mean(v * v, axis=1, keepdims=True)
            dn[r] = v * lax.rsqrt(sq + EPS) * gain
        nb[d] = dn[...].astype(BF16)
        if d == 0:
            mown[...] = mid[pl.ds(pl.multiple_of(tp * ROWS, 8), ROWS)]

    forward(0)
    pump(16)
    forward(1)
    pump(17)
    project(0)
    forward(3)
    pump(18)
    project(1)
    forward(2)
    pump(19)
    pump(20)
    project(3)
    pump(21)
    project(2)
    pump(22)
    pump(23)

    def block(d):
        g = nt(nb[d], wm[0:UNITS])
        u = nt(nb[d], wm[UNITS : 2 * UNITS])
        hid = (g / (1.0 + jnp.exp(-g)) * u).astype(BF16)
        for n in range(4):
            cols = slice(512 * n, 512 * n + 512)
            dn[:, cols] = jnp.dot(hid, wm[2 * UNITS : 3 * UNITS, cols], preferred_element_type=F32)
        for e in range(NX):
            xb = up(x, -e, NX)
            pown[d * NX + e] = dn[pl.ds(pl.multiple_of((xb * 2 + c) * ROWS, 8), ROWS)]
            dsend[d, e] = dn[pl.ds(pl.multiple_of((xb * 2 + 1 - c) * ROWS, 8), ROWS)].astype(BF16)
        go(dsend.at[d], drecv.at[d], dds.at[d], ddr.at[d], partner)

    HALF = DM // 2

    def first(d):
        yb = up(y, -d, NY)
        got(drecv.at[d], dds.at[d], ddr.at[d])
        for e in range(NX):
            v = pown[d * NX + e] + drecv[d, e].astype(F32)
            if e:
                asend[d, e - 1] = v[:, :HALF].astype(BF16)
            else:
                aown[d] = v[:, :HALF]
            if d:
                bsend[d - 1, e] = v[:, HALF:].astype(BF16)
            else:
                bown[e] = v[:, HALF:]
        if d:
            go(bsend.at[d - 1], brecv.at[d - 1], f2s.at[d - 1], f2r.at[d - 1], (z, yb, x, c))
        for e in range(1, NX):
            dev = (z, y, up(x, -e, NX), c)
            go(asend.at[d, e - 1], arecv.at[d, e - 1], f1s.at[d, e - 1], f1r.at[d, e - 1], dev)

    def second(d):
        v = aown[d]
        for e in range(1, NX):
            got(arecv.at[d, e - 1], f1s.at[d, e - 1], f1r.at[d, e - 1])
            v = v + arecv[d, e - 1].astype(F32)
        if d:
            a2send[d - 1] = v.astype(BF16)
            go(a2send.at[d - 1], a2recv.at[d - 1], f3s.at[d - 1], f3r.at[d - 1], (z, up(y, -d, NY), x, c))
        else:
            outa[...] = v

    block(2)
    block(1)
    first(2)
    block(3)
    first(1)
    block(0)
    first(3)
    second(2)
    first(0)
    second(1)
    second(3)
    for d in range(1, NY):
        got(brecv.at[d - 1], f2s.at[d - 1], f2r.at[d - 1])
    for e in range(NX):
        v = bown[e]
        for d in range(1, NY):
            v = v + brecv[d - 1, e].astype(F32)
        if e:
            b2send[e - 1] = v.astype(BF16)
            go(b2send.at[e - 1], b2recv.at[e - 1], f4s.at[e - 1], f4r.at[e - 1], (z, y, up(x, -e, NX), c))
        else:
            outb = v
    second(0)
    va = outa[...]
    for d in range(1, NY):
        got(a2recv.at[d - 1], f3s.at[d - 1], f3r.at[d - 1])
        va = va + a2recv[d - 1].astype(F32)
    out_ref[:, :HALF] = (mown[:, :HALF] + 0.5 * va).astype(BF16)
    for e in range(1, NX):
        got(b2recv.at[e - 1], f4s.at[e - 1], f4r.at[e - 1])
        outb = outb + b2recv[e - 1].astype(F32)
    out_ref[:, HALF:] = (mown[:, HALF:] + 0.5 * outb).astype(BF16)
    for cp in pending:
        cp.wait_send()


def body(queries, keys, values, q_gain, k_gain, w_out, residual, norm_gain, w_gate, w_up, w_down):
    first = (lax.axis_index("z") * NY + lax.axis_index("y")) * TOK
    positions = first + jnp.arange(TOK, dtype=jnp.int32)
    row_pos = (positions // GRID_W).astype(F32)
    col_pos = (positions % GRID_W).astype(F32)
    inv_freq = THETA ** (-jnp.arange(0, 32, 2, dtype=F32) / 32)
    ar = inv_freq[:, None] * row_pos[None, :]
    ac = inv_freq[:, None] * col_pos[None, :]
    tab = jnp.concatenate(
        [
            jnp.cos(ar), jnp.sin(ar), jnp.cos(ac), jnp.sin(ac),
            jnp.broadcast_to(q_gain[:, None], (64, TOK)),
            jnp.broadcast_to(k_gain[:, None], (64, TOK)),
        ],
        axis=0,
    )
    v = pltpu.VMEM
    dma = pltpu.SemaphoreType.DMA
    scratch = [
        v((NZ, TOK, 128), BF16),
        v((NY, TOK, 128), BF16),
        v((4 * TOK, 128), BF16),
        v((4 * TOK, 128), BF16),
        *[v((NY * TOK, 128), F32)] * 5,
        v((HID, 128), F32),
        v((NY, UNITS, 128), BF16),
        v((NY - 1, UNITS, 128), BF16),
        v((3 * UNITS, DM), BF16),
        v((1024, DM), BF16),
        v((NC, NY, NX, ROWS, DM), BF16),
        v((NY, TOK, 1024), BF16),
        v((3, TOK, 128), BF16), v((3, TOK, 128), BF16),
        v((3, 32, TOK), F32), v((3, 32, TOK), F32),
        v((TOK, DM), F32), v((NY, TOK, DM), BF16), v((TOK, DM), F32),
        v((16, ROWS, DM), F32),
        v((NY, NX, ROWS, DM), BF16), v((NY, NX, ROWS, DM), BF16),
        v((ROWS, DM), F32),
        v((4, 3, ROWS, DM // 2), BF16), v((4, 3, ROWS, DM // 2), BF16), v((4, ROWS, DM // 2), F32),
        v((3, 4, ROWS, DM // 2), BF16), v((3, 4, ROWS, DM // 2), BF16), v((4, ROWS, DM // 2), F32),
        *[v((3, ROWS, DM // 2), BF16)] * 4,
        v((ROWS, DM // 2), F32),
        dma((2, 8)), dma((2, 8)), dma((3,)), dma((3,)), dma((3,)), dma((3,)), dma((2, 3, 8)), dma((2, 3, 8)),
        dma((3,)), dma((3,)), dma((3,)), dma((3,)), dma((4,)), dma((4,)), dma((3,)), dma((3,)), dma((4,)), dma((4,)),
        dma((3,)), dma((3,)), dma((3,)), dma((3,)), dma((16,)), dma((16,)), dma((16,)), dma((16,)),
        dma((4,)), dma((4,)), dma((4, 3)), dma((4, 3)), *[dma((3,))] * 6,
    ]
    return pl.pallas_call(
        kernel,
        out_shape=jax.ShapeDtypeStruct((ROWS, DM), BF16),
        in_specs=[pl.BlockSpec(memory_space=pltpu.VMEM)] * 10,
        out_specs=pl.BlockSpec(memory_space=pltpu.VMEM),
        scratch_shapes=scratch,
        compiler_params=pltpu.CompilerParams(collective_id=0, has_side_effects=True, vmem_limit_bytes=60 * 1024 * 1024),
        name="layer",
    )(queries, keys.T, values.T, tab, w_gate, w_up, w_down.T, w_out, residual, norm_gain[None, :])


def solution(mesh):
    finer = Mesh(mesh.devices.reshape(NZ, NY, NX, NC), ("z", "y", "x", "c"))
    sp, tp, every = ("z", "y"), ("x", "c"), ("z", "y", "x", "c")
    placed = (
        P(sp, tp), P(sp, tp), P(sp, tp), P(), P(), P(tp, None), P(every, None), P(), P(sp, tp), P(sp, tp), P(tp, sp),
    )
    return jax.shard_map(body, mesh=finer, in_specs=placed, out_specs=P(every, None), check_vma=False)
```
